1024 devices in a mesh: ep: 64 (over z, core), tp: 16 (over y, x).
Axes of the slice: x: 4, y: 4, z: 32, core: 2. Of those that a mesh axis runs over, the one named last changes fastest.
Arguments:
- tokens: bfloat16 [4096, 2048], P('ep'), may hold values from -6 to 6
- mix_gain: float32 [2048], replicated, may hold values from 0.1 to 1.9
- w_in: bfloat16 [2048, 1024], P(None, 'tp'), may hold values from -0.125 to 0.125
- decay_re: float32 [64, 64], P('tp'), may hold values from -1 to -0.1
- freq: float32 [64, 64], P('tp'), may hold values from 0 to 100
- log_step: float32 [64], P('tp'), may hold values from -3.9 to 0
- in_re: bfloat16 [64, 16, 64], P('tp'), may hold values from -1 to 1
- in_im: bfloat16 [64, 16, 64], P('tp'), may hold values from -1 to 1
- out_re: bfloat16 [64, 16, 64], P('tp'), may hold values from -0.75 to 0.75
- out_im: bfloat16 [64, 16, 64], P('tp'), may hold values from -0.75 to 0.75
- skip: float32 [64, 16], P('tp'), may hold values from -4 to 4
- state_re: float32 [4096, 64, 64], P('ep', 'tp'), may hold values from -6 to 6
- state_im: float32 [4096, 64, 64], P('ep', 'tp'), may hold values from -6 to 6
- glu_weight: bfloat16 [1024, 1024], P(None, 'tp'), may hold values from -0.1875 to 0.1875
- glu_bias: float32 [1024], P('tp'), may hold values from -4 to 4
- out_weight: bfloat16 [1024, 2048], P('tp'), may hold values from -0.1875 to 0.1875
- ffn_gain: float32 [2048], replicated, may hold values from 0.1 to 1.9
- route: int32 [4096, 2], P('ep'), may hold values from 0 to 63, all different within a row; in each aligned block of 64 rows (0 to 63, 64 to 127, ...) at most 3 rows name the same one
- route_weight: float32 [4096, 2], P('ep'), may hold values from 0.2 to 1
- expert_gate: bfloat16 [64, 2048, 3584], P('ep', None, 'tp'), may hold values from -0.125 to 0.125
- expert_up: bfloat16 [64, 2048, 3584], P('ep', None, 'tp'), may hold values from -0.125 to 0.125
- expert_down: bfloat16 [64, 3584, 2048], P('ep', 'tp'), may hold values from -0.09375 to 0.09375
Outputs:
- mixed: bfloat16 [4096, 2048], P('ep', 'tp')
- new_re: float32 [4096, 64, 64], P('ep', 'tp')
- new_im: float32 [4096, 64, 64], P('ep', 'tp')
The draws below stay inside these ranges and needn't reach their ends.
Inputs may be any that keep to these rules, and one draw needn't show every extreme that they name: `route`: each row names 2 different experts. Within the 64 rows of one index of ep no expert is named more than 3 times, and in every draw some expert is named exactly 3 times by the rows of some index of ep.
All inputs are finite; a program needn't handle non-finite values.
Results may differ from the reference program's by a relative error of at most 0.015.
Values may be sent and summed in bfloat16 or wider, within the bound.
A program may use at most 32 MiB of HBM per device.

```python
import math
import jax
import jax.numpy as jnp
import numpy as np
from jax import lax

D = 2048
C = 1024
H = 16
P_SIZE = 64
FFE = 3584
TOPK = 2
SEQ_GRP = 64
G = 64
EXPERTS = 64
SEQS = 4096
CAP = 3
ROWS_E = 192
N_TP = 16


def levels(rng, shape, pieces, low, largest):
    def one(dim, blocks):
        heights = jax.random.uniform(jax.random.fold_in(jax.random.fold_in(rng, 6), dim), (blocks,), jnp.float32, low / len(pieces), largest / len(pieces))
        return jnp.repeat(jnp.exp(heights), shape[dim] // blocks).reshape((-1,) + (1,) * (len(shape) - dim - 1))

    level = one(*pieces[0])
    for cut in pieces[1:]:
        level = level * one(*cut)
    return level


def routed_block(key, own, number, rows, count, top, bound, lean):
    ranking = jax.random.permutation(key, count)
    crowded, usual = portions_of(count, rows * top, bound, lean, True), portions_of(count, rows * top, bound, lean, False)
    places = jnp.arange(count)

    def named(tallies, turn):
        used = int((tallies > 0).sum())
        fixed = max(1, used // 4)
        moved = fixed + (places - fixed + turn * (used - fixed)) % max(1, count - fixed)
        return jnp.zeros((count,), jnp.int32).at[ranking[jnp.where(places < fixed, places, moved)]].set(jnp.asarray(tallies, jnp.int32))

    tallies = jnp.where(number % 4 == 0, named(crowded, number // 4), named(usual, number - number // 4 - 1))
    mixed = jax.random.permutation(jax.random.fold_in(own, 3), count)
    donor, taker = mixed[0:count // 2 * 2:2], mixed[1:count // 2 * 2:2]
    margin = jnp.minimum(tallies[donor] - 1, bound - tallies[taker]) // 2
    margin = jnp.where((donor == ranking[0]) | (taker == ranking[0]) | (tallies[taker] == 0), 0, jnp.maximum(margin, 0))
    moved = jax.random.randint(jax.random.fold_in(own, 4), (count // 2,), 0, 1 << 20) % (margin + 1)
    tallies = tallies.at[donor].add(-moved).at[taker].add(moved)
    members = jnp.searchsorted(jnp.cumsum(tallies), jnp.arange(rows * top), side="right").astype(jnp.int32)
    listing = members.reshape(top, rows).T
    listing = listing[jax.random.permutation(jax.random.fold_in(own, 1), rows)]
    turn = jax.random.randint(jax.random.fold_in(own, 2), (rows, 1), 0, top)
    return jnp.take_along_axis(listing, (jnp.arange(top)[None, :] + turn) % top, axis=1)


def portions_of(amount, total, bound, slope, full):
    loads = [(1 << 20) // math.isqrt(rank ** slope) + 1 for rank in range(1, amount + 1)]
    largest = bound if full else min(bound, max(-(-total // amount), total * loads[0] // sum(loads)))
    least = 1 if total - largest >= amount - 1 else 0
    holding, spare = [largest] + [least] * (amount - 1), total - largest - least * (amount - 1)
    while spare > 0:
        candidates = [i for i in range(1, amount) if holding[i] < largest] or [i for i in range(1, amount) if holding[i] < bound]
        whole, budget = sum([loads[i] for i in candidates]), spare
        for i in candidates:
            addition = min(bound - holding[i], max(1, budget * loads[i] // whole), spare)
            holding[i] = holding[i] + addition
            spare = spare - addition
    return np.array(holding)


def bell_draw(rng, shape, spread, most, split=(), kind=jnp.bfloat16):
    level = levels(rng, shape, split, -0.22, 0.18) if split else 1.0
    entries = jax.random.normal(rng, shape, jnp.float32) * spread * level
    return jnp.minimum(jnp.maximum(entries, -most), most).astype(kind)


def setup_inputs(seed: int = 0) -> dict:
    splits = jax.random.split(jax.random.key(seed), 23)
    tokens = bell_draw(splits[0], (SEQS, D), 1.0, 6.0, ((0, 64),))
    mix_gain = jnp.clip(1.0 + 0.18 * jax.random.normal(splits[1], (D,), jnp.float32), 0.1, 1.9)
    w_in = bell_draw(splits[2], (D, C), D ** -0.5, 0.125, ((1, 16),))
    decay_re = jnp.clip(-1.0 + 0.9 * jax.random.uniform(splits[3], (G, P_SIZE), jnp.float32) ** levels(splits[3], (G, P_SIZE), ((0, 16),), -0.2, 0.2), -1.0, -0.1)
    freq = jnp.clip(100.0 * jax.random.uniform(splits[4], (G, P_SIZE), jnp.float32) ** levels(splits[4], (G, P_SIZE), ((0, 16),), -0.2, 0.2), 0.0, 100.0)
    log_step = jnp.clip(-3.9 + 3.9 * jax.random.uniform(splits[5], (G,), jnp.float32) ** levels(splits[5], (G,), ((0, 16),), -0.2, 0.2), -3.9, 0.0)
    in_re = bell_draw(splits[6], (G, H, P_SIZE), (2 * H) ** -0.5, 1.0, ((0, 16),))
    in_im = bell_draw(splits[7], (G, H, P_SIZE), (2 * H) ** -0.5, 1.0, ((0, 16),))
    out_re = bell_draw(splits[8], (G, H, P_SIZE), P_SIZE ** -0.5, 0.75, ((0, 16),))
    out_im = bell_draw(splits[9], (G, H, P_SIZE), P_SIZE ** -0.5, 0.75, ((0, 16),))
    skip = bell_draw(splits[10], (G, H), 1.0, 4.0, ((0, 16),), jnp.float32)
    state_re = bell_draw(splits[11], (SEQS, G, P_SIZE), 1.0, 6.0, ((0, 64), (1, 16)), jnp.float32)
    state_im = bell_draw(splits[12], (SEQS, G, P_SIZE), 1.0, 6.0, ((0, 64), (1, 16)), jnp.float32)
    glu_weight = bell_draw(splits[13], (C, C), C ** -0.5, 0.1875, ((1, 16),))
    glu_bias = bell_draw(splits[14], (C,), 1.0, 4.0, ((0, 16),), jnp.float32)
    out_weight = bell_draw(splits[15], (C, D), C ** -0.5, 0.1875, ((0, 16),))
    ffn_gain = jnp.clip(1.0 + 0.18 * jax.random.normal(splits[16], (D,), jnp.float32), 0.1, 1.9)
    route_keys = jax.random.split(jax.random.fold_in(splits[17], 1), SEQS // SEQ_GRP)
    route_turns = jax.random.permutation(jax.random.fold_in(splits[17], 3), SEQS // SEQ_GRP)
    route = jax.vmap(lambda own, number: routed_block(jax.random.fold_in(splits[17], 2), own, number, SEQ_GRP, EXPERTS, TOPK, CAP, 2))(route_keys, route_turns).reshape((SEQS, TOPK))
    route_weight = jnp.clip(0.2 + 0.8 * jax.random.uniform(splits[18], (SEQS, TOPK), jnp.float32) ** levels(splits[18], (SEQS, TOPK), ((0, 64),), -0.2, 0.2), 0.2, 1.0)
    expert_gate = bell_draw(splits[19], (EXPERTS, D, FFE), D ** -0.5, 0.125, ((0, 64), (2, 16)))
    expert_up = bell_draw(splits[20], (EXPERTS, D, FFE), D ** -0.5, 0.125, ((0, 64), (2, 16)))
    expert_down = bell_draw(splits[21], (EXPERTS, FFE, D), FFE ** -0.5, 0.09375, ((0, 64), (1, 16)))
    return {"tokens": tokens, "mix_gain": mix_gain, "w_in": w_in, "decay_re": decay_re, "freq": freq, "log_step": log_step, "in_re": in_re, "in_im": in_im, "out_re": out_re, "out_im": out_im, "skip": skip, "state_re": state_re, "state_im": state_im, "glu_weight": glu_weight, "glu_bias": glu_bias, "out_weight": out_weight, "ffn_gain": ffn_gain, "route": route, "route_weight": route_weight, "expert_gate": expert_gate, "expert_up": expert_up, "expert_down": expert_down}


norm_eps = 1e-06

def rms_scale(rows, gain):
    values = rows.astype(jnp.float32)
    scaled = values * lax.rsqrt(lax.optimization_barrier(jnp.mean(values * values, axis=-1, keepdims=True)) + norm_eps)
    return (scaled * gain).astype(jnp.bfloat16)

def split_sum(left, right, parts):
    width = left.shape[1] // parts
    lefts = jnp.moveaxis(left.reshape(left.shape[0], parts, width), 1, 0)
    rights = right.reshape(parts, width, right.shape[1])

    def add_block(total, pair):
        term = jnp.dot(pair[0], pair[1], preferred_element_type=jnp.float32).astype(jnp.bfloat16)
        term = lax.optimization_barrier(term)
        return (total + term.astype(jnp.float32), None)
    start = jnp.zeros((left.shape[0], right.shape[1]), jnp.float32)
    total, _ = lax.scan(add_block, start, (lefts, rights))
    return total

def state_step(inputs, state_re, state_im, decay_re, freq, log_step, in_re, in_im, out_re, out_im, skip):
    highest = lax.Precision.HIGHEST
    step = jnp.exp(log_step)[:, None]
    magnitude = jnp.exp(decay_re * step)
    turn_re = magnitude * jnp.cos(freq * step)
    turn_im = magnitude * jnp.sin(freq * step)
    denom = decay_re * decay_re + freq * freq
    coef_re = ((turn_re - 1.0) * decay_re + turn_im * freq) / denom
    coef_im = (turn_im * decay_re - (turn_re - 1.0) * freq) / denom
    values = inputs.astype(jnp.float32)
    drive_re = jnp.einsum('sgh,ghp->sgp', values, in_re.astype(jnp.float32), precision=highest)
    drive_im = jnp.einsum('sgh,ghp->sgp', values, in_im.astype(jnp.float32), precision=highest)
    push_re = coef_re * drive_re - coef_im * drive_im
    push_im = coef_re * drive_im + coef_im * drive_re
    new_re = turn_re * state_re - turn_im * state_im + push_re
    new_im = turn_re * state_im + turn_im * state_re + push_im
    read = jnp.einsum('ghp,sgp->sgh', out_re.astype(jnp.float32), new_re, precision=highest)
    read = read - jnp.einsum('ghp,sgp->sgh', out_im.astype(jnp.float32), new_im, precision=highest)
    read = read + skip * values
    return (read, new_re, new_im)

def reference(tokens, mix_gain, w_in, decay_re, freq, log_step, in_re, in_im, out_re, out_im, skip, state_re, state_im, glu_weight, glu_bias, out_weight, ffn_gain, route, route_weight, expert_gate, expert_up, expert_down):
    normed = rms_scale(tokens, mix_gain)
    drive = jnp.dot(normed, w_in, preferred_element_type=jnp.float32).astype(jnp.bfloat16)
    inputs = drive.reshape(SEQS, G, H)
    read, new_re, new_im = state_step(inputs, state_re, state_im, decay_re, freq, log_step, in_re, in_im, out_re, out_im, skip)
    mixed_in = jax.nn.gelu(read).reshape(SEQS, C).astype(jnp.bfloat16)
    gate = jnp.dot(mixed_in, glu_weight, preferred_element_type=jnp.float32) + glu_bias
    gated = (mixed_in.astype(jnp.float32) * jax.nn.sigmoid(gate)).astype(jnp.bfloat16)
    mix_total = split_sum(gated, out_weight, N_TP)
    resid = (tokens.astype(jnp.float32) + mix_total).astype(jnp.bfloat16)
    normed2 = rms_scale(resid, ffn_gain)
    flat_route = route.reshape(-1)
    flat_weight = route_weight.reshape(-1)

    def expert_pass(total, inputs_e):
        gate_w, up_w, down_w, index = inputs_e
        hits = flat_route == index
        picked = jnp.nonzero(hits, size=ROWS_E, fill_value=0)[0].astype(jnp.int32)
        valid = (jnp.arange(ROWS_E) < jnp.sum(hits.astype(jnp.int32))).astype(jnp.float32)
        token_ids = (picked // TOPK).astype(jnp.int32)
        rows = normed2[token_ids]
        gate_e = jnp.dot(rows, gate_w, preferred_element_type=jnp.float32)
        up_e = jnp.dot(rows, up_w, preferred_element_type=jnp.float32)
        hidden = (jax.nn.silu(gate_e) * up_e).astype(jnp.bfloat16)
        result = split_sum(hidden, down_w, N_TP).astype(jnp.bfloat16)
        weight = flat_weight[picked] * valid
        total = total.at[token_ids].add(weight[:, None] * result.astype(jnp.float32))
        return (total, None)
    start = resid.astype(jnp.float32)
    indices = jnp.arange(EXPERTS).astype(jnp.int32)
    total, _ = lax.scan(expert_pass, start, (expert_gate, expert_up, expert_down, indices))
    return (total.astype(jnp.bfloat16), new_re, new_im)
```

```python
import functools

import jax
import jax.numpy as jnp
from jax import lax
from jax.experimental import pallas as pl
from jax.experimental.pallas import tpu as pltpu
from jax.sharding import PartitionSpec as P

MESH = pl.DeviceIdType.MESH
F32 = jnp.float32
BF16 = jnp.bfloat16
norm_eps = 1e-06

CHUNKS = 4
SLOTS = 3
PAD = 4


def iota(shape, dim):
    return lax.broadcasted_iota(jnp.int32, shape, dim)


def mm(a, b):
    return jnp.dot(a, b, preferred_element_type=F32)


def mm_nt(a, b):
    return lax.dot_general(a, b, (((1,), (1,)), ((), ())), preferred_element_type=F32)


def ring_order(nz):
    order = [0]
    for k in range(1, nz // 2):
        order += [k, -k]
    return order + [nz // 2]


def kernel(
    nz,
    ntp,
    tokens_h,
    w_in_h,
    state_re_h,
    state_im_h,
    glu_h,
    out_w_h,
    gate_h,
    up_h,
    down_h,
    mix_gain,
    turn_re,
    turn_im,
    coef_re,
    coef_im,
    in_re,
    in_im,
    out_re,
    out_im,
    skip,
    glu_bias,
    ffn_gain,
    route_t,
    weight_t,
    mixed_o,
    new_re_o,
    new_im_o,
    tokens_v,
    w_in_v,
    state_re_v,
    state_im_v,
    glu_v,
    out_w_v,
    gate_v,
    up_v,
    down_v,
    sel_v,
    comb_v,
    mix_src,
    mix_buf,
    mix_all,
    part_src,
    part_buf,
    resid_v,
    out_msg,
    arr,
    rows_src,
    rows_buf,
    xn_v,
    down_src,
    down_buf,
    back_src,
    back_buf,
    ld_sem,
    send_sem,
    mix_sem,
    part_sem,
    arr_sem,
    rows_sem,
    down_sem,
    back_sem,
):
    ep = lax.axis_index("ep")
    tp = lax.axis_index("tp")
    z = ep // 2
    core = ep % 2
    experts = 2 * nz
    per = experts // CHUNKS
    crows = per * SLOTS
    seqs, width = tokens_v.shape
    order = ring_order(nz)
    place = {off % nz: i for i, off in enumerate(order)}

    def zdev(off, other):
        c = core if other == 0 else 1 - core
        return lax.rem(z + (off % nz), nz) * 2 + c

    def tdev(k):
        return lax.rem(tp + k, ntp)

    t_order = sorted(range(1, ntp), key=lambda k: -((k % 4 != 0) + (k // 4 != 0)))

    bar = pltpu.get_barrier_semaphore()
    for off in reversed(order):
        for other in (0, 1):
            if off == 0 and other == 0:
                continue
            pl.semaphore_signal(
                bar, inc=1, device_id=(zdev(off, other), tp), device_id_type=MESH
            )
    for k in range(1, ntp):
        pl.semaphore_signal(bar, inc=1, device_id=(ep, tdev(k)), device_id_type=MESH)

    loads = [
        pltpu.make_async_copy(src, dst, ld_sem.at[i])
        for i, (src, dst) in enumerate(
            [
                (tokens_h, tokens_v),
                (w_in_h, w_in_v),
                (state_re_h, state_re_v),
                (state_im_h, state_im_v),
                (glu_h, glu_v),
                (out_w_h, out_w_v),
                (gate_h.at[0], gate_v),
                (up_h.at[0], up_v),
                (down_h.at[0], down_v),
            ]
        )
    ]
    for copy in loads:
        copy.start()

    lines = experts * PAD
    expert_of = iota((lines, seqs), 0) // PAD
    slot_of = (iota((lines, seqs), 0) % PAD).astype(F32)
    before = (iota((seqs, seqs), 0) < iota((seqs, seqs), 1)).astype(BF16)
    taken = jnp.zeros((lines, 1), F32)
    sel = jnp.zeros((lines, seqs), F32)
    comb = jnp.zeros((lines, seqs), F32)
    for k in range(route_t.shape[0]):
        hits = (route_t[k : k + 1, :] == expert_of).astype(F32)
        rank = mm(hits.astype(BF16), before) + taken
        mine = jnp.where(rank == slot_of, hits, 0.0)
        taken = taken + jnp.sum(hits, axis=1, keepdims=True)
        sel = sel + mine
        comb = comb + mine * weight_t[k : k + 1, :]
    sel_v[...] = sel.astype(BF16)
    comb_hi = comb.astype(BF16)
    comb_lo = (comb - comb_hi.astype(F32)).astype(BF16)
    same = (iota((seqs, seqs), 0) == iota((seqs, seqs), 1)).astype(BF16)
    comb_v[0] = mm_nt(same, comb_hi).astype(BF16)
    comb_v[1] = mm_nt(same, comb_lo).astype(BF16)

    loads[0].wait()
    values = tokens_v[...].astype(F32)
    scale = lax.rsqrt(jnp.mean(values * values, axis=-1, keepdims=True) + norm_eps)
    normed = (values * scale * mix_gain[...]).astype(BF16)
    loads[1].wait()
    drive = mm(normed, w_in_v[...]).astype(BF16)
    loads[2].wait()
    loads[3].wait()
    chans = drive.shape[1]
    groups = turn_re.shape[0]
    chan_group = iota((chans, in_re.shape[1]), 0) // (chans // groups)
    read = skip[...] * drive.astype(F32)
    for g in range(groups):
        own = chan_group == g
        zero = jnp.zeros(own.shape, BF16)
        drive_re = mm(drive, jnp.where(own, in_re[...], zero))
        drive_im = mm(drive, jnp.where(own, in_im[...], zero))
        tr, ti = turn_re[g : g + 1, :], turn_im[g : g + 1, :]
        cr, ci = coef_re[g : g + 1, :], coef_im[g : g + 1, :]
        sr, si = state_re_v[:, g, :], state_im_v[:, g, :]
        nr = tr * sr - ti * si + (cr * drive_re - ci * drive_im)
        ni = tr * si + ti * sr + (cr * drive_im + ci * drive_re)
        new_re_o[:, g, :] = nr
        new_im_o[:, g, :] = ni
        o_re = jnp.where(own, out_re[...], zero)
        o_im = jnp.where(own, out_im[...], zero)
        for val, o_mat, sign in ((nr, o_re, 1.0), (ni, o_im, -1.0)):
            hi = val.astype(BF16)
            lo = (val - hi.astype(F32)).astype(BF16)
            read = read + sign * (mm_nt(hi, o_mat) + mm_nt(lo, o_mat))
    mixed_in = jax.nn.gelu(read).astype(BF16)

    half = seqs // 2
    row, col = iota((chans, 2 * chans), 0), iota((chans, 2 * chans), 1)
    left = (row == col).astype(BF16)
    right = (row + chans == col).astype(BF16)
    packed = mm(mixed_in[:half], left) + mm(mixed_in[half:], right)
    mix_src[...] = packed.astype(BF16)
    mix_buf[tp] = packed.astype(BF16)

    pl.semaphore_wait(bar, 2 * nz - 1 + ntp - 1)

    def to_group(src_of, dst, send, recv):
        for k in t_order:
            t = tdev(k)
            pltpu.make_async_remote_copy(
                src_ref=src_of(t),
                dst_ref=dst,
                send_sem=send,
                recv_sem=recv,
                device_id=(ep, t),
                device_id_type=MESH,
            ).start()

    def arrived(ref, sem):
        pltpu.make_async_copy(ref, ref, sem).wait()

    to_group(lambda t: mix_src, mix_buf.at[tp], send_sem.at[0], mix_sem)
    loads[4].wait()
    loads[5].wait()
    arrived(mix_buf.at[pl.ds(0, ntp - 1)], mix_sem)
    lane = iota((half, 2 * chans), 1)
    gate = jnp.zeros((seqs, chans), F32)
    for t in range(ntp):
        block = mix_buf[t]
        zero = jnp.zeros(block.shape, BF16)
        mix_all[0:half] = jnp.where(lane < chans, block, zero)
        mix_all[half:seqs] = jnp.where(lane < chans, zero, block)
        w = glu_v[t * chans : (t + 1) * chans, :]
        gate = gate + mm(mix_all[...], jnp.concatenate([w, w], axis=0))
    gated = (mixed_in.astype(F32) * jax.nn.sigmoid(gate + glu_bias[...])).astype(BF16)
    local = width // ntp
    for t in range(ntp):
        part = mm(gated, out_w_v[:, t * local : (t + 1) * local])
        part_src[t] = part.astype(BF16)
    part_buf[tp] = part_src[tp]
    to_group(lambda t: part_src.at[t], part_buf.at[tp], send_sem.at[1], part_sem)
    arrived(part_buf.at[pl.ds(0, ntp - 1)], part_sem)
    total = tokens_v[:, pl.ds(pl.multiple_of(tp * local, local), local)].astype(F32)
    mix_total = part_buf[0].astype(F32)
    for t in range(1, ntp):
        mix_total = mix_total + part_buf[t].astype(F32)
    resid = (total + mix_total).astype(BF16)
    resid_v[...] = resid

    out_msg[...] = mm(sel_v[...], resid).astype(BF16).reshape(experts, PAD, local)
    for off in reversed(order):
        for other in (0, 1):
            if off == 0 and other == 0:
                continue
            dst = zdev(off, other)
            pos = 2 * place[-off % nz] + other
            pltpu.make_async_remote_copy(
                src_ref=out_msg.at[dst],
                dst_ref=arr.at[pos],
                send_sem=send_sem.at[2],
                recv_sem=arr_sem.at[pos // per],
                device_id=(dst, tp),
                device_id_type=MESH,
            ).start()
    arr[0] = out_msg[ep]

    line, spot = iota((crows, per * PAD), 0), iota((crows, per * PAD), 1)
    compact = ((line % per) * PAD + line // per == spot).astype(BF16)
    spot2, line2 = iota((per * PAD, crows), 0), iota((per * PAD, crows), 1)
    spread = ((line2 % per) * PAD + line2 // per == spot2).astype(BF16)

    def gather(c):
        first = 1 if c == 0 else 0
        arrived(arr.at[pl.ds(c * per + first, per - first)], arr_sem.at[c])
        block = arr[c * per : (c + 1) * per].reshape(per * PAD, local)
        rows = mm(compact, block).astype(BF16)
        rows_src[c] = rows
        rows_buf[c, tp] = rows
        to_group(lambda t: rows_src.at[c], rows_buf.at[c, tp], send_sem.at[3 + c], rows_sem.at[c])

    def expert(c):
        arrived(rows_buf.at[c, pl.ds(0, ntp - 1)], rows_sem.at[c])
        squares = jnp.zeros((crows, local), F32)
        for t in range(ntp):
            v = rows_buf[c, t].astype(F32)
            squares = squares + v * v
        norm = lax.rsqrt(jnp.sum(squares, axis=1, keepdims=True) / width + norm_eps)
        for t in range(ntp):
            v = rows_buf[c, t].astype(F32)
            gain = ffn_gain[:, t * local : (t + 1) * local]
            xn_v[:, t * local : (t + 1) * local] = (v * norm * gain).astype(BF16)
        if c == 0:
            for i in (6, 7, 8):
                loads[i].wait()
        rows = xn_v[...]
        hidden = (jax.nn.silu(mm(rows, gate_v[...])) * mm(rows, up_v[...])).astype(BF16)
        for t in range(ntp):
            down_src[c, t] = mm(hidden, down_v[:, t * local : (t + 1) * local]).astype(BF16)
        down_buf[c, tp] = down_src[c, tp]
        to_group(
            lambda t: down_src.at[c, t],
            down_buf.at[c, tp],
            send_sem.at[3 + CHUNKS + c],
            down_sem.at[c],
        )

    def give_back(c):
        arrived(down_buf.at[c, pl.ds(0, ntp - 1)], down_sem.at[c])
        rows = down_buf[c, 0].astype(F32)
        for t in range(1, ntp):
            rows = rows + down_buf[c, t].astype(F32)
        rows = mm(spread, rows.astype(BF16)).astype(BF16)
        back_src[c * per : (c + 1) * per] = rows.reshape(per, PAD, local)
        for pos in reversed(range(c * per, (c + 1) * per)):
            if pos == 0:
                back_buf[ep] = back_src[0]
                continue
            dst = zdev(order[pos // 2], pos % 2)
            pltpu.make_async_remote_copy(
                src_ref=back_src.at[pos],
                dst_ref=back_buf.at[ep],
                send_sem=send_sem.at[3 + 2 * CHUNKS],
                recv_sem=back_sem,
                device_id=(dst, tp),
                device_id_type=MESH,
            ).start()

    gather(0)
    gather(1)
    expert(0)
    gather(2)
    expert(1)
    gather(3)
    expert(2)
    give_back(0)
    expert(3)
    give_back(1)
    give_back(2)
    give_back(3)

    arrived(back_buf.at[pl.ds(0, experts - 1)], back_sem)
    back = back_buf[...].reshape(lines, local)
    summed = mm(comb_v[0], back) + mm(comb_v[1], back)
    mixed_o[...] = (resid_v[...].astype(F32) + summed).astype(BF16)

    others = ntp - 1
    arrived(mix_buf.at[pl.ds(0, others)], send_sem.at[0])
    arrived(part_buf.at[pl.ds(0, others)], send_sem.at[1])
    arrived(arr.at[pl.ds(0, experts - 1)], send_sem.at[2])
    for c in range(CHUNKS):
        arrived(rows_buf.at[c, pl.ds(0, others)], send_sem.at[3 + c])
        arrived(down_buf.at[c, pl.ds(0, others)], send_sem.at[3 + CHUNKS + c])
    arrived(back_buf.at[pl.ds(0, experts - 1)], send_sem.at[3 + 2 * CHUNKS])


def local(
    nz,
    ntp,
    tokens,
    mix_gain,
    w_in,
    decay_re,
    freq,
    log_step,
    in_re,
    in_im,
    out_re,
    out_im,
    skip,
    state_re,
    state_im,
    glu_weight,
    glu_bias,
    out_weight,
    ffn_gain,
    route,
    route_weight,
    expert_gate,
    expert_up,
    expert_down,
):
    step = jnp.exp(log_step)[:, None]
    magnitude = jnp.exp(decay_re * step)
    turn_re = magnitude * jnp.cos(freq * step)
    turn_im = magnitude * jnp.sin(freq * step)
    denom = decay_re * decay_re + freq * freq
    coef_re = ((turn_re - 1.0) * decay_re + turn_im * freq) / denom
    coef_im = (turn_im * decay_re - (turn_re - 1.0) * freq) / denom

    seqs, width = tokens.shape
    chans = w_in.shape[1]
    states = decay_re.shape[1]
    loc = width // ntp
    experts = 2 * nz
    per = experts // CHUNKS
    crows = per * SLOTS
    flat = lambda m: m.reshape(chans, states)
    row = lambda v: v.reshape(1, -1)

    def vmem(*shape, dtype=BF16):
        return pltpu.VMEM(shape, dtype)

    dma = pltpu.SemaphoreType.DMA
    any_spec = pl.BlockSpec(memory_space=pl.ANY)
    vmem_spec = pl.BlockSpec(memory_space=pltpu.VMEM)
    return pl.pallas_call(
        functools.partial(kernel, nz, ntp),
        out_shape=(
            jax.ShapeDtypeStruct((seqs, loc), BF16),
            jax.ShapeDtypeStruct(state_re.shape, F32),
            jax.ShapeDtypeStruct(state_im.shape, F32),
        ),
        in_specs=[any_spec] * 9 + [vmem_spec] * 14,
        out_specs=(vmem_spec,) * 3,
        scratch_shapes=[
            vmem(*tokens.shape),
            vmem(*w_in.shape),
            vmem(*state_re.shape, dtype=F32),
            vmem(*state_im.shape, dtype=F32),
            vmem(*glu_weight.shape),
            vmem(*out_weight.shape),
            vmem(*expert_gate.shape[1:]),
            vmem(*expert_up.shape[1:]),
            vmem(*expert_down.shape[1:]),
            vmem(experts * PAD, seqs),
            vmem(2, seqs, experts * PAD),
            vmem(seqs // 2, 2 * chans),
            vmem(ntp, seqs // 2, 2 * chans),
            vmem(seqs, 2 * chans),
            vmem(ntp, seqs, loc),
            vmem(ntp, seqs, loc),
            vmem(seqs, loc),
            vmem(experts, PAD, loc),
            vmem(experts, PAD, loc),
            vmem(CHUNKS, crows, loc),
            vmem(CHUNKS, ntp, crows, loc),
            vmem(crows, width),
            vmem(CHUNKS, ntp, crows, loc),
            vmem(CHUNKS, ntp, crows, loc),
            vmem(experts, PAD, loc),
            vmem(experts, PAD, loc),
            dma((9,)),
            dma((4 + 2 * CHUNKS,)),
            dma,
            dma,
            dma((CHUNKS,)),
            dma((CHUNKS,)),
            dma((CHUNKS,)),
            dma,
        ],
        compiler_params=pltpu.CompilerParams(collective_id=0, has_side_effects=True),
    )(
        tokens,
        w_in,
        state_re,
        state_im,
        glu_weight,
        out_weight,
        expert_gate,
        expert_up,
        expert_down,
        row(mix_gain),
        turn_re,
        turn_im,
        coef_re,
        coef_im,
        flat(in_re),
        flat(in_im),
        flat(out_re),
        flat(out_im),
        row(skip),
        row(glu_bias),
        row(ffn_gain),
        route.T,
        route_weight.T,
    )


def solution(mesh):
    ep, tp = mesh.axis_names
    placed = (
        P(ep, None),
        P(),
        P(None, tp),
        P(tp, None),
        P(tp, None),
        P(tp),
        P(tp, None, None),
        P(tp, None, None),
        P(tp, None, None),
        P(tp, None, None),
        P(tp, None),
        P(ep, tp, None),
        P(ep, tp, None),
        P(None, tp),
        P(tp),
        P(tp, None),
        P(),
        P(ep, None),
        P(ep, None),
        P(ep, None, tp),
        P(ep, None, tp),
        P(ep, tp, None),
    )
    return jax.shard_map(
        functools.partial(local, mesh.shape[ep] // 2, mesh.shape[tp]),
        mesh=mesh,
        in_specs=placed,
        out_specs=(P(ep, tp), P(ep, tp, None), P(ep, tp, None)),
        check_vma=False,
    )
```

```python
import functools

import jax
import jax.numpy as jnp
from jax import lax
from jax.experimental import pallas as pl
from jax.experimental.pallas import tpu as pltpu
from jax.sharding import PartitionSpec as P

MESH = pl.DeviceIdType.MESH
F32 = jnp.float32
BF16 = jnp.bfloat16
norm_eps = 1e-06

CHUNKS = 4
SLOTS = 3
PAD = 4


def iota(shape, dim):
    return lax.broadcasted_iota(jnp.int32, shape, dim)


def mm(a, b):
    return jnp.dot(a, b, preferred_element_type=F32)


def mm_nt(a, b):
    return lax.dot_general(a, b, (((1,), (1,)), ((), ())), preferred_element_type=F32)


def ring_order(nz):
    order = [0]
    for k in range(1, nz // 2):
        order += [k, -k]
    return order + [nz // 2]


INPUTS = (
    "route_t",
    "weight_t",
    "log_step",
    "decay_re",
    "freq",
    "skip",
    "in_re",
    "in_im",
    "out_re",
    "out_im",
    "mix_gain",
    "tokens",
    "w_in_t",
    "state_re",
    "state_im",
    "glu_bias",
    "glu_t",
    "out_w",
    "ffn_gain",
    "gate_t",
    "up_t",
    "down",
)


def kernel(nz, ntp, *refs):
    hbm = dict(zip(INPUTS, refs))
    refs = refs[len(INPUTS) :]
    mixed_o, new_re_o, new_im_o = refs[:3]
    v = dict(zip(INPUTS, refs[3:]))
    (
        sel_v,
        comb_v,
        glu_s,
        mix_src,
        mix_buf,
        mix_all,
        part_src,
        part_buf,
        resid_v,
        out_msg,
        arr,
        rows_src,
        rows_buf,
        xn_v,
        down_src,
        down_buf,
        back_src,
        back_buf,
        ld_sem,
        send_sem,
        mix_sem,
        part_sem,
        arr_sem,
        rows_sem,
        down_sem,
        back_sem,
        near_sem,
    ) = refs[3 + len(INPUTS) :]
    ep = lax.axis_index("ep")
    tp = lax.axis_index("tp")
    z = ep // 2
    core = ep % 2
    experts = 2 * nz
    per = experts // CHUNKS
    crows = per * SLOTS
    seqs, width = v["tokens"].shape
    order = ring_order(nz)

    def zdev(off, other):
        c = core if other == 0 else 1 - core
        return lax.rem(z + (off % nz), nz) * 2 + c

    def tdev(k):
        return lax.rem(tp + k, ntp)

    def signal(sem, dst):
        pl.semaphore_signal(sem, inc=1, device_id=dst, device_id_type=MESH)

    reach = nz // 8
    near = [(off, o) for off in order if abs(off) <= reach for o in (0, 1)]
    near.remove((0, 0))
    bar = pltpu.get_barrier_semaphore()
    for off, other in reversed(near):
        signal(bar, (zdev(off, other), tp))
    for k in range(1, ntp):
        signal(bar, (ep, tdev(k)))

    loads = {
        n: pltpu.make_async_copy(hbm[n], v[n], ld_sem.at[i]) for i, n in enumerate(INPUTS)
    }
    for n in INPUTS:
        loads[n].start()

    def loaded(*names):
        for n in names:
            loads[n].wait()

    loaded("log_step", "decay_re", "freq")
    decay_re, freq = v["decay_re"][...], v["freq"][...]
    groups, states = decay_re.shape
    group = iota((groups, states), 0)
    log_step = jnp.zeros((groups, states), F32)
    for g in range(groups):
        log_step = jnp.where(group == g, v["log_step"][0:1, g : g + 1], log_step)
    step = jnp.exp(log_step)
    magnitude = jnp.exp(decay_re * step)
    turn_re = magnitude * jnp.cos(freq * step)
    turn_im = magnitude * jnp.sin(freq * step)
    denom = decay_re * decay_re + freq * freq
    coef_re = ((turn_re - 1.0) * decay_re + turn_im * freq) / denom
    coef_im = (turn_im * decay_re - (turn_re - 1.0) * freq) / denom

    loaded("skip", "in_re", "in_im", "out_re", "out_im", "mix_gain", "tokens")
    values = v["tokens"][...].astype(F32)
    scale = lax.rsqrt(jnp.mean(values * values, axis=-1, keepdims=True) + norm_eps)
    normed = (values * scale * v["mix_gain"][...]).astype(BF16)
    loaded("w_in_t")
    drive = mm_nt(normed, v["w_in_t"][...]).astype(BF16)
    chans = drive.shape[1]
    places = chans // groups
    chan_group = iota((chans, states), 0) // places
    spread_h = (iota((places, chans), 0) == iota((places, chans), 1) % places).astype(BF16)
    skip_rows = jnp.zeros((groups, chans), F32)
    rest = v["skip"][...]
    for _ in range(3):
        piece = rest.astype(BF16)
        skip_rows = skip_rows + mm(piece, spread_h)
        rest = rest - piece.astype(F32)
    of_group = iota((groups, chans), 0) == iota((groups, chans), 1) // places
    skip = jnp.sum(jnp.where(of_group, skip_rows, 0.0), axis=0, keepdims=True)
    read = skip * drive.astype(F32)
    loaded("state_re", "state_im")
    for g in range(groups):
        own = chan_group == g
        zero = jnp.zeros(own.shape, BF16)
        drive_re = mm(drive, jnp.where(own, v["in_re"][...], zero))
        drive_im = mm(drive, jnp.where(own, v["in_im"][...], zero))
        tr, ti = turn_re[g : g + 1, :], turn_im[g : g + 1, :]
        cr, ci = coef_re[g : g + 1, :], coef_im[g : g + 1, :]
        sr, si = v["state_re"][:, g, :], v["state_im"][:, g, :]
        nr = tr * sr - ti * si + (cr * drive_re - ci * drive_im)
        ni = tr * si + ti * sr + (cr * drive_im + ci * drive_re)
        new_re_o[:, g, :] = nr
        new_im_o[:, g, :] = ni
        o_re = jnp.where(own, v["out_re"][...], zero)
        o_im = jnp.where(own, v["out_im"][...], zero)
        for val, o_mat, sign in ((nr, o_re, 1.0), (ni, o_im, -1.0)):
            hi = val.astype(BF16)
            lo = (val - hi.astype(F32)).astype(BF16)
            read = read + sign * (mm_nt(hi, o_mat) + mm_nt(lo, o_mat))
    mixed_in = jax.nn.gelu(read).astype(BF16)

    half = seqs // 2
    row, col = iota((chans, 2 * chans), 0), iota((chans, 2 * chans), 1)
    left = (row == col).astype(BF16)
    right = (row + chans == col).astype(BF16)
    packed = mm(mixed_in[:half], left) + mm(mixed_in[half:], right)
    mix_src[...] = packed.astype(BF16)
    mix_buf[tp] = packed.astype(BF16)

    pl.semaphore_wait(bar, len(near) + ntp - 1)
    def pass_on(i):
        for off in (reach << i, -(reach << i)):
            signal(near_sem.at[i], (zdev(off, 0), tp))

    pass_on(0)

    t_order = sorted(range(1, ntp), key=lambda k: -((k % 4 != 0) + (k // 4 != 0)))

    def to_group(src_of, dst, send, recv):
        for k in t_order:
            t = tdev(k)
            pltpu.make_async_remote_copy(
                src_ref=src_of(t),
                dst_ref=dst,
                send_sem=send,
                recv_sem=recv,
                device_id=(ep, t),
                device_id_type=MESH,
            ).start()

    def arrived(ref, sem):
        pltpu.make_async_copy(ref, ref, sem).wait()

    to_group(lambda t: mix_src, mix_buf.at[tp], send_sem.at[0], mix_sem)

    loaded("glu_t", "glu_bias", "out_w")
    wide = 2 * chans
    same = (iota((wide, wide), 0) == iota((wide, wide), 1)).astype(BF16)
    for p in range(ntp // 2):
        w = mm_nt(same, v["glu_t"][:, p * wide : (p + 1) * wide]).astype(BF16)
        for i in (0, 1):
            t = 2 * p + i
            for j in (0, 1):
                at = t * wide + j * chans
                glu_s[at : at + chans, :] = w[i * chans : (i + 1) * chans, :]

    arrived(mix_buf.at[pl.ds(0, ntp - 1)], mix_sem)
    pl.semaphore_wait(near_sem.at[0], 2)
    pass_on(1)
    lane = iota((half, wide), 1)
    for t in range(ntp):
        block = mix_buf[t]
        zero = jnp.zeros(block.shape, BF16)
        mix_all[0:half, t * wide : (t + 1) * wide] = jnp.where(lane < chans, block, zero)
        mix_all[half:seqs, t * wide : (t + 1) * wide] = jnp.where(lane < chans, zero, block)
    gate = mm(mix_all[...], glu_s[...]) + v["glu_bias"][...]
    gated = (mixed_in.astype(F32) * jax.nn.sigmoid(gate)).astype(BF16)
    local = width // ntp
    step_t = 4
    for t0 in range(0, ntp, step_t):
        part = mm(gated, v["out_w"][:, t0 * local : (t0 + step_t) * local]).astype(BF16)
        for i in range(step_t):
            part_src[t0 + i] = part[:, i * local : (i + 1) * local]
    to_group(lambda t: part_src.at[t], part_buf.at[tp], send_sem.at[1], part_sem)
    part_buf[tp] = part_src[tp]

    loaded("route_t", "weight_t")
    lines = experts * PAD
    expert_of = iota((lines, seqs), 0) // PAD
    slot_of = (iota((lines, seqs), 0) % PAD).astype(F32)
    before = (iota((seqs, seqs), 0) < iota((seqs, seqs), 1)).astype(BF16)
    taken = jnp.zeros((lines, 1), F32)
    sel = jnp.zeros((lines, seqs), F32)
    comb = jnp.zeros((lines, seqs), F32)
    for k in range(v["route_t"].shape[0]):
        hits = (v["route_t"][k : k + 1, :] == expert_of).astype(F32)
        rank = mm(hits.astype(BF16), before) + taken
        mine = jnp.where(rank == slot_of, hits, 0.0)
        taken = taken + jnp.sum(hits, axis=1, keepdims=True)
        sel = sel + mine
        comb = comb + mine * v["weight_t"][k : k + 1, :]
    sel_v[...] = sel.astype(BF16)
    comb_hi = comb.astype(BF16)
    comb_lo = (comb - comb_hi.astype(F32)).astype(BF16)
    eye = (iota((seqs, seqs), 0) == iota((seqs, seqs), 1)).astype(BF16)
    comb_v[0] = mm_nt(eye, comb_hi).astype(BF16)
    comb_v[1] = mm_nt(eye, comb_lo).astype(BF16)

    total = v["tokens"][:, pl.ds(pl.multiple_of(tp * local, local), local)].astype(F32)
    arrived(part_buf.at[pl.ds(0, ntp - 1)], part_sem)
    mix_total = part_buf[0].astype(F32)
    for t in range(1, ntp):
        mix_total = mix_total + part_buf[t].astype(F32)
    resid = (total + mix_total).astype(BF16)
    resid_v[...] = resid

    out_msg[...] = mm(sel_v[...], resid).astype(BF16).reshape(experts, PAD, local)
    pl.semaphore_wait(near_sem.at[1], 2)
    chunk = z // (nz // CHUNKS)
    for off in reversed(order):
        for other in (0, 1):
            if off == 0 and other == 0:
                continue
            dst = zdev(off, other)
            pltpu.make_async_remote_copy(
                src_ref=out_msg.at[dst],
                dst_ref=arr.at[ep],
                send_sem=send_sem.at[2],
                recv_sem=arr_sem.at[chunk],
                device_id=(dst, tp),
                device_id_type=MESH,
            ).start()
    pltpu.make_async_copy(out_msg.at[ep], arr.at[ep], arr_sem.at[chunk]).start()

    line, spot = iota((crows, per * PAD), 0), iota((crows, per * PAD), 1)
    compact = ((line % per) * PAD + line // per == spot).astype(BF16)
    spot2, line2 = iota((per * PAD, crows), 0), iota((per * PAD, crows), 1)
    spread = ((line2 % per) * PAD + line2 // per == spot2).astype(BF16)

    def gather(c):
        arrived(arr.at[pl.ds(c * per, per)], arr_sem.at[c])
        block = arr[c * per : (c + 1) * per].reshape(per * PAD, local)
        rows = mm(compact, block).astype(BF16)
        rows_src[c] = rows
        to_group(lambda t: rows_src.at[c], rows_buf.at[c, tp], send_sem.at[3 + c], rows_sem.at[c])
        rows_buf[c, tp] = rows

    def expert(c, first=False):
        arrived(rows_buf.at[c, pl.ds(0, ntp - 1)], rows_sem.at[c])
        if first:
            loaded("ffn_gain")
        squares = jnp.zeros((crows, local), F32)
        for t in range(ntp):
            x = rows_buf[c, t].astype(F32)
            squares = squares + x * x
        norm = lax.rsqrt(jnp.sum(squares, axis=1, keepdims=True) / width + norm_eps)
        for t in range(ntp):
            x = rows_buf[c, t].astype(F32)
            gain = v["ffn_gain"][:, t * local : (t + 1) * local]
            xn_v[:, t * local : (t + 1) * local] = (x * norm * gain).astype(BF16)
        if first:
            loaded("gate_t", "up_t", "down")
        rows = xn_v[...]
        hidden = jax.nn.silu(mm_nt(rows, v["gate_t"][...])) * mm_nt(rows, v["up_t"][...])
        hidden = hidden.astype(BF16)
        for t0 in range(0, ntp, step_t):
            y = mm(hidden, v["down"][:, t0 * local : (t0 + step_t) * local]).astype(BF16)
            for i in range(step_t):
                down_src[c, t0 + i] = y[:, i * local : (i + 1) * local]
        to_group(
            lambda t: down_src.at[c, t],
            down_buf.at[c, tp],
            send_sem.at[3 + CHUNKS + c],
            down_sem.at[c],
        )
        down_buf[c, tp] = down_src[c, tp]

    def give_back(c):
        arrived(down_buf.at[c, pl.ds(0, ntp - 1)], down_sem.at[c])
        rows = down_buf[c, 0].astype(F32)
        for t in range(1, ntp):
            rows = rows + down_buf[c, t].astype(F32)
        rows = mm(spread, rows.astype(BF16)).astype(BF16)
        back_src[c * per : (c + 1) * per] = rows.reshape(per, PAD, local)
        for dst in range(c * per, (c + 1) * per):

            @pl.when(ep != dst)
            def _():
                pltpu.make_async_remote_copy(
                    src_ref=back_src.at[dst],
                    dst_ref=back_buf.at[ep],
                    send_sem=send_sem.at[3 + 2 * CHUNKS],
                    recv_sem=back_sem,
                    device_id=(dst, tp),
                    device_id_type=MESH,
                ).start()

        @pl.when(chunk == c)
        def _():
            pltpu.make_async_copy(back_src.at[ep], back_buf.at[ep], back_sem).start()

    gather(0)
    gather(1)
    gather(2)
    expert(0, True)
    expert(2)
    gather(3)
    expert(1)
    give_back(0)
    expert(3)
    give_back(1)
    give_back(2)
    give_back(3)

    arrived(back_buf, back_sem)
    back = back_buf[...].reshape(lines, local)
    summed = mm(comb_v[0], back) + mm(comb_v[1], back)
    mixed_o[...] = (resid_v[...].astype(F32) + summed).astype(BF16)

    others = ntp - 1
    arrived(mix_buf.at[pl.ds(0, others)], send_sem.at[0])
    arrived(part_buf.at[pl.ds(0, others)], send_sem.at[1])
    arrived(arr.at[pl.ds(0, experts - 1)], send_sem.at[2])
    for c in range(CHUNKS):
        arrived(rows_buf.at[c, pl.ds(0, others)], send_sem.at[3 + c])
        arrived(down_buf.at[c, pl.ds(0, others)], send_sem.at[3 + CHUNKS + c])
    arrived(back_buf.at[pl.ds(0, experts - 1)], send_sem.at[3 + 2 * CHUNKS])


def local(
    nz,
    ntp,
    tokens,
    mix_gain,
    w_in,
    decay_re,
    freq,
    log_step,
    in_re,
    in_im,
    out_re,
    out_im,
    skip,
    state_re,
    state_im,
    glu_weight,
    glu_bias,
    out_weight,
    ffn_gain,
    route,
    route_weight,
    expert_gate,
    expert_up,
    expert_down,
):
    seqs, width = tokens.shape
    chans = w_in.shape[1]
    states = decay_re.shape[1]
    loc = width // ntp
    experts = 2 * nz
    per = experts // CHUNKS
    crows = per * SLOTS
    flat = lambda m: m.reshape(chans, states)
    row = lambda x: x.reshape(1, -1)

    def vmem(*shape, dtype=BF16):
        return pltpu.VMEM(shape, dtype)

    inputs = dict(
        route_t=route.T,
        weight_t=route_weight.T,
        log_step=row(log_step),
        decay_re=decay_re,
        freq=freq,
        skip=skip,
        in_re=flat(in_re),
        in_im=flat(in_im),
        out_re=flat(out_re),
        out_im=flat(out_im),
        mix_gain=row(mix_gain),
        tokens=tokens,
        w_in_t=w_in.T,
        state_re=state_re,
        state_im=state_im,
        glu_bias=row(glu_bias),
        glu_t=glu_weight.T,
        out_w=out_weight,
        ffn_gain=row(ffn_gain),
        gate_t=expert_gate[0].T,
        up_t=expert_up[0].T,
        down=expert_down[0],
    )
    operands = [inputs[n] for n in INPUTS]
    dma = pltpu.SemaphoreType.DMA
    any_spec = pl.BlockSpec(memory_space=pl.ANY)
    vmem_spec = pl.BlockSpec(memory_space=pltpu.VMEM)
    outs = (
        jax.ShapeDtypeStruct((seqs, loc), BF16),
        jax.ShapeDtypeStruct(state_re.shape, F32),
        jax.ShapeDtypeStruct(state_im.shape, F32),
    )
    made = pl.pallas_call(
        functools.partial(kernel, nz, ntp),
        out_shape=tuple(pltpu.VMEM(o.shape, o.dtype) for o in outs),
        in_specs=[any_spec] * len(operands),
        out_specs=(vmem_spec,) * 3,
        scratch_shapes=[vmem(*x.shape, dtype=x.dtype) for x in operands]
        + [
            vmem(experts * PAD, seqs),
            vmem(2, seqs, experts * PAD),
            vmem(ntp * 2 * chans, chans),
            vmem(seqs // 2, 2 * chans),
            vmem(ntp, seqs // 2, 2 * chans),
            vmem(seqs, ntp * 2 * chans),
            vmem(ntp, seqs, loc),
            vmem(ntp, seqs, loc),
            vmem(seqs, loc),
            vmem(experts, PAD, loc),
            vmem(experts, PAD, loc),
            vmem(CHUNKS, crows, loc),
            vmem(CHUNKS, ntp, crows, loc),
            vmem(crows, width),
            vmem(CHUNKS, ntp, crows, loc),
            vmem(CHUNKS, ntp, crows, loc),
            vmem(experts, PAD, loc),
            vmem(experts, PAD, loc),
            dma((len(operands),)),
            dma((4 + 2 * CHUNKS,)),
            dma,
            dma,
            dma((CHUNKS,)),
            dma((CHUNKS,)),
            dma((CHUNKS,)),
            dma,
            pltpu.SemaphoreType.REGULAR((2,)),
        ],
        compiler_params=pltpu.CompilerParams(collective_id=0, has_side_effects=True),
    )(*operands)
    return made


def solution(mesh):
    ep, tp = mesh.axis_names
    placed = (
        P(ep, None),
        P(),
        P(None, tp),
        P(tp, None),
        P(tp, None),
        P(tp),
        P(tp, None, None),
        P(tp, None, None),
        P(tp, None, None),
        P(tp, None, None),
        P(tp, None),
        P(ep, tp, None),
        P(ep, tp, None),
        P(None, tp),
        P(tp),
        P(tp, None),
        P(),
        P(ep, None),
        P(ep, None),
        P(ep, None, tp),
        P(ep, None, tp),
        P(ep, tp, None),
    )
    return jax.shard_map(
        functools.partial(local, mesh.shape[ep] // 2, mesh.shape[tp]),
        mesh=mesh,
        in_specs=placed,
        out_specs=(P(ep, tp), P(ep, tp, None), P(ep, tp, None)),
        check_vma=False,
    )
```

```python
import functools

import jax
import jax.numpy as jnp
from jax import lax
from jax.experimental import pallas as pl
from jax.experimental.pallas import tpu as pltpu
from jax.sharding import PartitionSpec as P

MESH = pl.DeviceIdType.MESH
F32 = jnp.float32
BF16 = jnp.bfloat16
norm_eps = 1e-06

CHUNKS = 4
SLOTS = 3
PAD = 4


def iota(shape, dim):
    return lax.broadcasted_iota(jnp.int32, shape, dim)


def mm(a, b):
    return jnp.dot(a, b, preferred_element_type=F32)


def mm_nt(a, b):
    return lax.dot_general(a, b, (((1,), (1,)), ((), ())), preferred_element_type=F32)


INPUTS = (
    "route_t",
    "weight_t",
    "log_step",
    "decay_re",
    "freq",
    "skip",
    "in_re",
    "in_im",
    "out_re",
    "out_im",
    "mix_gain",
    "tokens",
    "w_in_t",
    "state_re",
    "state_im",
    "glu_bias",
    "glu_t",
    "out_w",
    "ffn_gain",
    "gate_t",
    "up_t",
    "down",
)


def kernel(nz, ntp, *refs):
    hbm = dict(zip(INPUTS, refs))
    refs = refs[len(INPUTS) :]
    mixed_o, new_re_o, new_im_o = refs[:3]
    v = dict(zip(INPUTS, refs[3:]))
    (
        sel_v,
        comb_v,
        glu_s,
        mix_src,
        mix_buf,
        mix_all,
        part_src,
        part_buf,
        resid_v,
        out_msg,
        arr,
        rows_src,
        rows_buf,
        xn_v,
        down_src,
        down_buf,
        back_src,
        back_buf,
        ld_sem,
        send_sem,
        mix_sem,
        part_sem,
        arr_sem,
        rows_sem,
        down_sem,
        back_sem,
        near_sem,
        hand,
        hand_sem,
        wrap_sem,
    ) = refs[3 + len(INPUTS) :]
    ep = lax.axis_index("ep")
    tp = lax.axis_index("tp")
    z = ep // 2
    core = ep % 2
    experts = 2 * nz
    per = experts // CHUNKS
    crows = per * SLOTS
    seqs, width = v["tokens"].shape

    def zdev(off, other):
        c = core if other == 0 else 1 - core
        return lax.rem(z + (off % nz), nz) * 2 + c

    def tdev(k):
        return lax.rem(tp + k, ntp)

    def signal(sem, dst):
        pl.semaphore_signal(sem, inc=1, device_id=dst, device_id_type=MESH)

    reach = nz // 4
    has_prev = 1 - (nz - z) // nz
    has_next = 1 - (z + 1) // nz
    is_last = (z + reach) // nz
    bar = pltpu.get_barrier_semaphore()

    def both(off):
        for other in (0, 1):
            signal(bar, (zdev(off, other), tp))

    for d in range(reach, 0, -1):
        pl.when(z < d)(functools.partial(both, -d))
    pl.when(z > 0)(functools.partial(both, -1))
    pl.when(z < nz - 1)(functools.partial(both, 1))
    signal(bar, (zdev(0, 1), tp))
    for k in range(1, ntp):
        signal(bar, (ep, tdev(k)))

    loads = {
        n: pltpu.make_async_copy(hbm[n], v[n], ld_sem.at[i]) for i, n in enumerate(INPUTS)
    }
    for n in INPUTS:
        loads[n].start()

    def loaded(*names):
        for n in names:
            loads[n].wait()

    loaded("log_step", "decay_re", "freq")
    decay_re, freq = v["decay_re"][...], v["freq"][...]
    groups, states = decay_re.shape
    group = iota((groups, states), 0)
    log_step = jnp.zeros((groups, states), F32)
    for g in range(groups):
        log_step = jnp.where(group == g, v["log_step"][0:1, g : g + 1], log_step)
    step = jnp.exp(log_step)
    magnitude = jnp.exp(decay_re * step)
    turn_re = magnitude * jnp.cos(freq * step)
    turn_im = magnitude * jnp.sin(freq * step)
    denom = decay_re * decay_re + freq * freq
    coef_re = ((turn_re - 1.0) * decay_re + turn_im * freq) / denom
    coef_im = (turn_im * decay_re - (turn_re - 1.0) * freq) / denom

    loaded("skip", "in_re", "in_im", "out_re", "out_im", "mix_gain", "tokens")
    values = v["tokens"][...].astype(F32)
    scale = lax.rsqrt(jnp.mean(values * values, axis=-1, keepdims=True) + norm_eps)
    normed = (values * scale * v["mix_gain"][...]).astype(BF16)
    loaded("w_in_t")
    drive = mm_nt(normed, v["w_in_t"][...]).astype(BF16)
    chans = drive.shape[1]
    places = chans // groups
    chan_group = iota((chans, states), 0) // places
    spread_h = (iota((places, chans), 0) == iota((places, chans), 1) % places).astype(BF16)
    skip_rows = jnp.zeros((groups, chans), F32)
    rest = v["skip"][...]
    for _ in range(3):
        piece = rest.astype(BF16)
        skip_rows = skip_rows + mm(piece, spread_h)
        rest = rest - piece.astype(F32)
    of_group = iota((groups, chans), 0) == iota((groups, chans), 1) // places
    skip = jnp.sum(jnp.where(of_group, skip_rows, 0.0), axis=0, keepdims=True)
    read = skip * drive.astype(F32)
    loaded("state_re", "state_im")
    for g in range(groups):
        own = chan_group == g
        zero = jnp.zeros(own.shape, BF16)
        drive_re = mm(drive, jnp.where(own, v["in_re"][...], zero))
        drive_im = mm(drive, jnp.where(own, v["in_im"][...], zero))
        tr, ti = turn_re[g : g + 1, :], turn_im[g : g + 1, :]
        cr, ci = coef_re[g : g + 1, :], coef_im[g : g + 1, :]
        sr, si = v["state_re"][:, g, :], v["state_im"][:, g, :]
        nr = tr * sr - ti * si + (cr * drive_re - ci * drive_im)
        ni = tr * si + ti * sr + (cr * drive_im + ci * drive_re)
        new_re_o[:, g, :] = nr
        new_im_o[:, g, :] = ni
        o_re = jnp.where(own, v["out_re"][...], zero)
        o_im = jnp.where(own, v["out_im"][...], zero)
        for val, o_mat, sign in ((nr, o_re, 1.0), (ni, o_im, -1.0)):
            hi = val.astype(BF16)
            lo = (val - hi.astype(F32)).astype(BF16)
            read = read + sign * (mm_nt(hi, o_mat) + mm_nt(lo, o_mat))
    mixed_in = jax.nn.gelu(read).astype(BF16)

    half = seqs // 2
    row, col = iota((chans, 2 * chans), 0), iota((chans, 2 * chans), 1)
    left = (row == col).astype(BF16)
    right = (row + chans == col).astype(BF16)
    packed = mm(mixed_in[:half], left) + mm(mixed_in[half:], right)
    mix_src[...] = packed.astype(BF16)
    mix_buf[tp] = packed.astype(BF16)

    firsts = 2 * is_last * (z - (nz - reach) + 1)
    pl.semaphore_wait(bar, ntp + 2 * has_prev + 2 * has_next + firsts)

    rounds = (1, 2, 4)

    def pass_on(i):
        r = rounds[i]

        @pl.when(z >= r)
        def _():
            signal(near_sem.at[i], (zdev(-r, 0), tp))

        @pl.when(z < nz - r)
        def _():
            signal(near_sem.at[i], (zdev(r, 0), tp))

    def heard(i):
        r = rounds[i]
        pl.semaphore_wait(near_sem.at[i], 2 - (nz - 1 - z + r) // nz - (z + r) // nz)

    pass_on(0)
    for d in range(reach, 0, -1):

        @pl.when(z >= nz - d)
        def _():
            signal(wrap_sem, (zdev(d, 0), tp))

    t_order = sorted(range(1, ntp), key=lambda k: -((k % 4 != 0) + (k // 4 != 0)))

    def to_group(src_of, dst, send, recv):
        for k in t_order:
            t = tdev(k)
            pltpu.make_async_remote_copy(
                src_ref=src_of(t),
                dst_ref=dst,
                send_sem=send,
                recv_sem=recv,
                device_id=(ep, t),
                device_id_type=MESH,
            ).start()

    def arrived(ref, sem):
        pltpu.make_async_copy(ref, ref, sem).wait()

    to_group(lambda t: mix_src, mix_buf.at[tp], send_sem.at[0], mix_sem)

    loaded("glu_t", "glu_bias", "out_w")
    wide = 2 * chans
    same = (iota((wide, wide), 0) == iota((wide, wide), 1)).astype(BF16)
    for p in range(ntp // 2):
        w = mm_nt(same, v["glu_t"][:, p * wide : (p + 1) * wide]).astype(BF16)
        for i in (0, 1):
            t = 2 * p + i
            for j in (0, 1):
                at = t * wide + j * chans
                glu_s[at : at + chans, :] = w[i * chans : (i + 1) * chans, :]

    heard(0)
    pass_on(1)
    heard(1)
    pass_on(2)
    arrived(mix_buf.at[pl.ds(0, ntp - 1)], mix_sem)
    lane = iota((half, wide), 1)
    for t in range(ntp):
        block = mix_buf[t]
        zero = jnp.zeros(block.shape, BF16)
        mix_all[0:half, t * wide : (t + 1) * wide] = jnp.where(lane < chans, block, zero)
        mix_all[half:seqs, t * wide : (t + 1) * wide] = jnp.where(lane < chans, zero, block)
    gate = mm(mix_all[...], glu_s[...]) + v["glu_bias"][...]
    gated = (mixed_in.astype(F32) * jax.nn.sigmoid(gate)).astype(BF16)
    local = width // ntp
    step_t = 4
    for t0 in range(0, ntp, step_t):
        part = mm(gated, v["out_w"][:, t0 * local : (t0 + step_t) * local]).astype(BF16)
        for i in range(step_t):
            part_src[t0 + i] = part[:, i * local : (i + 1) * local]
    to_group(lambda t: part_src.at[t], part_buf.at[tp], send_sem.at[1], part_sem)
    part_buf[tp] = part_src[tp]

    loaded("route_t", "weight_t")
    lines = experts * PAD
    expert_of = iota((lines, seqs), 0) // PAD
    slot_of = (iota((lines, seqs), 0) % PAD).astype(F32)
    before = (iota((seqs, seqs), 0) < iota((seqs, seqs), 1)).astype(BF16)
    taken = jnp.zeros((lines, 1), F32)
    sel = jnp.zeros((lines, seqs), F32)
    comb = jnp.zeros((lines, seqs), F32)
    for k in range(v["route_t"].shape[0]):
        hits = (v["route_t"][k : k + 1, :] == expert_of).astype(F32)
        rank = mm(hits.astype(BF16), before) + taken
        mine = jnp.where(rank == slot_of, hits, 0.0)
        taken = taken + jnp.sum(hits, axis=1, keepdims=True)
        sel = sel + mine
        comb = comb + mine * v["weight_t"][k : k + 1, :]
    sel_v[...] = sel.astype(BF16)
    comb_hi = comb.astype(BF16)
    comb_lo = (comb - comb_hi.astype(F32)).astype(BF16)
    eye = (iota((seqs, seqs), 0) == iota((seqs, seqs), 1)).astype(BF16)
    comb_v[0] = mm_nt(eye, comb_hi).astype(BF16)
    comb_v[1] = mm_nt(eye, comb_lo).astype(BF16)

    total = v["tokens"][:, pl.ds(pl.multiple_of(tp * local, local), local)].astype(F32)
    arrived(part_buf.at[pl.ds(0, ntp - 1)], part_sem)
    mix_total = part_buf[0].astype(F32)
    for t in range(1, ntp):
        mix_total = mix_total + part_buf[t].astype(F32)
    resid = (total + mix_total).astype(BF16)
    resid_v[...] = resid

    out_msg[...] = mm(sel_v[...], resid).astype(BF16).reshape(experts, PAD, local)
    heard(2)
    chunk = z // (nz // CHUNKS)
    out_sem = send_sem.at[2]

    def send(src, dst, sem, other_sem, ring):
        pltpu.make_async_remote_copy(
            src_ref=src,
            dst_ref=dst,
            send_sem=other_sem,
            recv_sem=sem,
            device_id=(ring, tp),
            device_id_type=MESH,
        ).start()

    far = (nz // 2 - reach, nz // 2 - 1 - reach)
    start = (0, 2 * far[0])

    def outbound(way):
        sign = 1 - 2 * way
        via = zdev(sign * reach, 0)
        for i in reversed(range(2 * far[way])):
            dst = zdev(sign * (reach + i // 2 + 1), i % 2)
            send(out_msg.at[dst], hand.at[start[way] + i], hand_sem.at[way], out_sem, via)
        for d in range(reach, 0, -1):
            for other in (0, 1):
                dst = zdev(sign * d, other)
                send(out_msg.at[dst], arr.at[ep], arr_sem.at[chunk], out_sem, dst)

    def hand_on(way):
        sign = 1 - 2 * way
        src = zdev(-sign * reach, 0)
        theirs = arr_sem.at[src // per]
        arrived(hand.at[pl.ds(start[way], 2 * far[way])], hand_sem.at[way])
        for i in reversed(range(2 * far[way])):
            dst = zdev(sign * (i // 2 + 1), i % 2)
            send(hand.at[start[way] + i], arr.at[src], theirs, send_sem.at[4 + 2 * CHUNKS], dst)

    outbound(0)
    dst = zdev(0, 1)
    send(out_msg.at[dst], arr.at[ep], arr_sem.at[chunk], out_sem, dst)
    pltpu.make_async_copy(out_msg.at[ep], arr.at[ep], arr_sem.at[chunk]).start()

    @pl.when(z < reach)
    def _():
        pl.semaphore_wait(wrap_sem, reach - z)

    outbound(1)
    middle = jnp.logical_and(z >= nz // 4, z < nz - nz // 4)

    def hand_on_first(second):
        @pl.when(middle)
        def _():
            hand_on(1 if second else 0)

        @pl.when(jnp.logical_not(middle))
        def _():
            hand_on(0 if second else 1)

    line, spot = iota((crows, per * PAD), 0), iota((crows, per * PAD), 1)
    compact = ((line % per) * PAD + line // per == spot).astype(BF16)
    spot2, line2 = iota((per * PAD, crows), 0), iota((per * PAD, crows), 1)
    spread = ((line2 % per) * PAD + line2 // per == spot2).astype(BF16)

    def gather(c):
        arrived(arr.at[pl.ds(c * per, per)], arr_sem.at[c])
        block = arr[c * per : (c + 1) * per].reshape(per * PAD, local)
        rows = mm(compact, block).astype(BF16)
        rows_src[c] = rows
        to_group(lambda t: rows_src.at[c], rows_buf.at[c, tp], send_sem.at[3 + c], rows_sem.at[c])
        rows_buf[c, tp] = rows

    def expert(c, first=False):
        arrived(rows_buf.at[c, pl.ds(0, ntp - 1)], rows_sem.at[c])
        if first:
            loaded("ffn_gain")
        squares = jnp.zeros((crows, local), F32)
        for t in range(ntp):
            x = rows_buf[c, t].astype(F32)
            squares = squares + x * x
        norm = lax.rsqrt(jnp.sum(squares, axis=1, keepdims=True) / width + norm_eps)
        for t in range(ntp):
            x = rows_buf[c, t].astype(F32)
            gain = v["ffn_gain"][:, t * local : (t + 1) * local]
            xn_v[:, t * local : (t + 1) * local] = (x * norm * gain).astype(BF16)
        if first:
            loaded("gate_t", "up_t", "down")
        rows = xn_v[...]
        hidden = jax.nn.silu(mm_nt(rows, v["gate_t"][...])) * mm_nt(rows, v["up_t"][...])
        hidden = hidden.astype(BF16)
        for t0 in range(0, ntp, step_t):
            y = mm(hidden, v["down"][:, t0 * local : (t0 + step_t) * local]).astype(BF16)
            for i in range(step_t):
                down_src[c, t0 + i] = y[:, i * local : (i + 1) * local]
        to_group(
            lambda t: down_src.at[c, t],
            down_buf.at[c, tp],
            send_sem.at[3 + CHUNKS + c],
            down_sem.at[c],
        )
        down_buf[c, tp] = down_src[c, tp]

    def give_back(c):
        arrived(down_buf.at[c, pl.ds(0, ntp - 1)], down_sem.at[c])
        rows = down_buf[c, 0].astype(F32)
        for t in range(1, ntp):
            rows = rows + down_buf[c, t].astype(F32)
        rows = mm(spread, rows.astype(BF16)).astype(BF16)
        back_src[c * per : (c + 1) * per] = rows.reshape(per, PAD, local)
        for dst in range(c * per, (c + 1) * per):

            @pl.when(ep != dst)
            def _():
                pltpu.make_async_remote_copy(
                    src_ref=back_src.at[dst],
                    dst_ref=back_buf.at[ep],
                    send_sem=send_sem.at[3 + 2 * CHUNKS],
                    recv_sem=back_sem,
                    device_id=(dst, tp),
                    device_id_type=MESH,
                ).start()

        @pl.when(chunk == c)
        def _():
            pltpu.make_async_copy(back_src.at[ep], back_buf.at[ep], back_sem).start()

    hand_on_first(False)
    gather(0)
    hand_on_first(True)
    expert(0, True)
    gather(1)
    gather(2)
    give_back(0)
    gather(3)
    expert(1)
    expert(2)
    expert(3)
    give_back(1)
    give_back(2)
    give_back(3)

    arrived(back_buf, back_sem)
    back = back_buf[...].reshape(lines, local)
    summed = mm(comb_v[0], back) + mm(comb_v[1], back)
    mixed_o[...] = (resid_v[...].astype(F32) + summed).astype(BF16)

    others = ntp - 1
    arrived(mix_buf.at[pl.ds(0, others)], send_sem.at[0])
    arrived(part_buf.at[pl.ds(0, others)], send_sem.at[1])
    arrived(arr.at[pl.ds(0, experts - 1)], send_sem.at[2])
    for c in range(CHUNKS):
        arrived(rows_buf.at[c, pl.ds(0, others)], send_sem.at[3 + c])
        arrived(down_buf.at[c, pl.ds(0, others)], send_sem.at[3 + CHUNKS + c])
    arrived(back_buf.at[pl.ds(0, experts - 1)], send_sem.at[3 + 2 * CHUNKS])
    arrived(hand, send_sem.at[4 + 2 * CHUNKS])


def write_out(*refs):
    sems = refs[6]
    copies = [pltpu.make_async_copy(refs[i], refs[3 + i], sems.at[i]) for i in range(3)]
    for copy in copies:
        copy.start()
    for copy in copies:
        copy.wait()


def local(
    nz,
    ntp,
    tokens,
    mix_gain,
    w_in,
    decay_re,
    freq,
    log_step,
    in_re,
    in_im,
    out_re,
    out_im,
    skip,
    state_re,
    state_im,
    glu_weight,
    glu_bias,
    out_weight,
    ffn_gain,
    route,
    route_weight,
    expert_gate,
    expert_up,
    expert_down,
):
    seqs, width = tokens.shape
    chans = w_in.shape[1]
    states = decay_re.shape[1]
    loc = width // ntp
    experts = 2 * nz
    per = experts // CHUNKS
    crows = per * SLOTS
    flat = lambda m: m.reshape(chans, states)
    row = lambda x: x.reshape(1, -1)

    def vmem(*shape, dtype=BF16):
        return pltpu.VMEM(shape, dtype)

    inputs = dict(
        route_t=route.T,
        weight_t=route_weight.T,
        log_step=row(log_step),
        decay_re=decay_re,
        freq=freq,
        skip=skip,
        in_re=flat(in_re),
        in_im=flat(in_im),
        out_re=flat(out_re),
        out_im=flat(out_im),
        mix_gain=row(mix_gain),
        tokens=tokens,
        w_in_t=w_in.T,
        state_re=state_re,
        state_im=state_im,
        glu_bias=row(glu_bias),
        glu_t=glu_weight.T,
        out_w=out_weight,
        ffn_gain=row(ffn_gain),
        gate_t=expert_gate[0].T,
        up_t=expert_up[0].T,
        down=expert_down[0],
    )
    operands = [inputs[n] for n in INPUTS]
    dma = pltpu.SemaphoreType.DMA
    any_spec = pl.BlockSpec(memory_space=pl.ANY)
    vmem_spec = pl.BlockSpec(memory_space=pltpu.VMEM)
    outs = (
        jax.ShapeDtypeStruct((seqs, loc), BF16),
        jax.ShapeDtypeStruct(state_re.shape, F32),
        jax.ShapeDtypeStruct(state_im.shape, F32),
    )
    made = pl.pallas_call(
        functools.partial(kernel, nz, ntp),
        out_shape=tuple(pltpu.VMEM(o.shape, o.dtype) for o in outs),
        in_specs=[any_spec] * len(operands),
        out_specs=(vmem_spec,) * 3,
        scratch_shapes=[vmem(*x.shape, dtype=x.dtype) for x in operands]
        + [
            vmem(experts * PAD, seqs),
            vmem(2, seqs, experts * PAD),
            vmem(ntp * 2 * chans, chans),
            vmem(seqs // 2, 2 * chans),
            vmem(ntp, seqs // 2, 2 * chans),
            vmem(seqs, ntp * 2 * chans),
            vmem(ntp, seqs, loc),
            vmem(ntp, seqs, loc),
            vmem(seqs, loc),
            vmem(experts, PAD, loc),
            vmem(experts, PAD, loc),
            vmem(CHUNKS, crows, loc),
            vmem(CHUNKS, ntp, crows, loc),
            vmem(crows, width),
            vmem(CHUNKS, ntp, crows, loc),
            vmem(CHUNKS, ntp, crows, loc),
            vmem(experts, PAD, loc),
            vmem(experts, PAD, loc),
            dma((len(operands),)),
            dma((5 + 2 * CHUNKS,)),
            dma,
            dma,
            dma((CHUNKS,)),
            dma((CHUNKS,)),
            dma((CHUNKS,)),
            dma,
            pltpu.SemaphoreType.REGULAR((3,)),
            vmem(4 * (nz // 4) - 2, PAD, loc),
            dma((2,)),
            pltpu.SemaphoreType.REGULAR,
        ],
        compiler_params=pltpu.CompilerParams(collective_id=0, has_side_effects=True),
    )(*operands)
    return pl.pallas_call(
        write_out,
        out_shape=outs,
        in_specs=[vmem_spec] * 3,
        out_specs=(any_spec,) * 3,
        scratch_shapes=[dma((3,))],
    )(*[pltpu.with_memory_space_constraint(x, pltpu.VMEM) for x in made])


def solution(mesh):
    ep, tp = mesh.axis_names
    placed = (
        P(ep, None),
        P(),
        P(None, tp),
        P(tp, None),
        P(tp, None),
        P(tp),
        P(tp, None, None),
        P(tp, None, None),
        P(tp, None, None),
        P(tp, None, None),
        P(tp, None),
        P(ep, tp, None),
        P(ep, tp, None),
        P(None, tp),
        P(tp),
        P(tp, None),
        P(),
        P(ep, None),
        P(ep, None),
        P(ep, None, tp),
        P(ep, None, tp),
        P(ep, tp, None),
    )
    return jax.shard_map(
        functools.partial(local, mesh.shape[ep] // 2, mesh.shape[tp]),
        mesh=mesh,
        in_specs=placed,
        out_specs=(P(ep, tp), P(ep, tp, None), P(ep, tp, None)),
        check_vma=False,
    )
```
